256 devices in a mesh: grp: 2 (over y), ep: 64 (over z, x), tp: 2 (over core).
Axes of the slice: x: 4, y: 2, z: 16, core: 2. Of those that a mesh axis runs over, the one named last changes fastest.
The devices are a block of a 4x16x16 slice.
Arguments:
- tokens: bfloat16 [32768, 2048], P(('grp', 'ep', 'tp')), parts along dimension 0, may hold values from -6 to 6
- norm_gain: float32 [2048], replicated, may hold values from 0.1 to 1.9
- expert_ids: int32 [32768, 2], P(('grp', 'ep', 'tp')), parts along dimension 0, may hold values from 0 to 31, all different within a row; in each aligned block of 128 rows (0 to 127, 128 to 255, ...) at most 10 rows name the same one
- route_weights: float32 [32768, 2], P(('grp', 'ep', 'tp')), parts along dimension 0, may hold values from 0.1 to 0.9
- w_gate: bfloat16 [2048, 114688], P(None, ('ep', 'tp')), may hold values from -0.125 to 0.125
- w_up: bfloat16 [2048, 114688], P(None, ('ep', 'tp')), may hold values from -0.125 to 0.125
- w_down: bfloat16 [114688, 2048], P(('ep', 'tp')), may hold values from -0.09375 to 0.09375
Outputs:
- mixed_out: bfloat16 [32768, 2048], P(('grp', 'ep', 'tp')), parts along dimension 0
The draws below stay inside these ranges and needn't reach their ends.
There are 2 independent parts, one for each index of `grp`. The reference program is written for one: setup_inputs(seed, part) draws one part's arguments, and reference() takes and returns one part's arrays. A program takes and returns all parts, laid end to end along the dimension named above; an argument that names none is the same for every part. Nothing has to cross between parts.
Inputs may be any that keep to these rules, and one draw needn't show every extreme that they name: `expert_ids`: each row names 2 different experts. Among the rows of one device no expert is named more than 10 times, and in every draw some expert is named exactly 10 times by one device's rows.
All inputs are finite; a program needn't handle non-finite values.
Results may differ from the reference program's by a relative error of at most 0.01.
Values may be sent and summed in bfloat16 or wider, within the bound.
No kernel may reach another device: no remote copies, remote signals or barrier semaphores. Data moves between devices by JAX's collectives and lax.ppermute only.
A program may use at most 128 MiB of HBM per device.

```python
import math
import jax
import jax.numpy as jnp
import numpy as np
from jax import lax

D = 2048
FF = 3584
TOP_K = 2
TOK_DEV = 128
EXPERTS = 32
CAP = 10
TOKENS = 16384
N_TP = 2


def level_of(stream_key, extent, pieces, low, largest):
    loudness = 1.0
    for dim, blocks in pieces:
        heights = jax.random.uniform(jax.random.fold_in(jax.random.fold_in(stream_key, 6), dim), (blocks,), jnp.float32, low / len(pieces), largest / len(pieces))
        loudness = loudness * jnp.repeat(jnp.exp(heights), extent[dim] // blocks).reshape((-1,) + (1,) * (len(extent) - 1 - dim))
    return loudness


def routed_block(stream_key, own, number, rows, amount, top, reach, slope):
    order = jax.random.permutation(stream_key, amount)
    heavy_load, common = shares(amount, rows * top, reach, slope, True), shares(amount, rows * top, reach, slope, False)
    places = jnp.arange(amount)

    def named(tallies, turn):
        used = int((tallies > 0).sum())
        fixed = max(1, used // 4)
        passed = fixed + (places - fixed + turn * (used - fixed)) % max(1, amount - fixed)
        return jnp.zeros((amount,), jnp.int32).at[order[jnp.where(places < fixed, places, passed)]].set(jnp.asarray(tallies, jnp.int32))

    tallies = jnp.where(number % 4 == 0, named(heavy_load, number // 4), named(common, number - number // 4 - 1))
    mixed = jax.random.permutation(jax.random.fold_in(own, 3), amount)
    donor, taker = mixed[0:amount // 2 * 2:2], mixed[1:amount // 2 * 2:2]
    margin = jnp.minimum(tallies[donor] - 1, reach - tallies[taker]) // 2
    margin = jnp.where((donor == order[0]) | (taker == order[0]) | (tallies[taker] == 0), 0, jnp.maximum(margin, 0))
    passed = jax.random.randint(jax.random.fold_in(own, 4), (amount // 2,), 0, 1 << 20) % (margin + 1)
    tallies = tallies.at[donor].add(-passed).at[taker].add(passed)
    members = jnp.searchsorted(jnp.cumsum(tallies), jnp.arange(rows * top), side="right").astype(jnp.int32)
    table = members.reshape(top, rows).T
    table = table[jax.random.permutation(jax.random.fold_in(own, 1), rows)]
    turn = jax.random.randint(jax.random.fold_in(own, 2), (rows, 1), 0, top)
    return jnp.take_along_axis(table, (jnp.arange(top)[None, :] + turn) % top, axis=1)


def shares(count, total, reach, lean, full):
    portions = [(1 << 20) // math.isqrt(rank ** lean) + 1 for rank in range(1, count + 1)]
    largest = reach if full else min(reach, max(-(-total // count), total * portions[0] // sum(portions)))
    least = 1 if total - largest >= count - 1 else 0
    given, surplus = [largest] + [least] * (count - 1), total - largest - least * (count - 1)
    while surplus > 0:
        free = [i for i in range(1, count) if given[i] < largest] or [i for i in range(1, count) if given[i] < reach]
        whole, budget = sum([portions[i] for i in free]), surplus
        for i in free:
            addition = min(reach - given[i], max(1, budget * portions[i] // whole), surplus)
            given[i] = given[i] + addition
            surplus = surplus - addition
    return np.array(given)


def noise(rng, shape, scale, reach, shards=(), kind=jnp.bfloat16):
    drawn = jax.random.normal(rng, shape, jnp.float32) * scale
    if len(shards) > 0:
        drawn = level_of(rng, shape, shards, -0.22, 0.18) * drawn
    return jnp.clip(drawn, min=-reach, max=reach).astype(kind)


def setup_inputs(seed: int = 0, part: int = 0) -> dict:
    arg_keys = jax.random.split(jax.random.key(seed), 8)
    part_splits = jax.random.split(jax.random.fold_in(arg_keys[7], part), 8)
    tokens = noise(part_splits[0], (TOKENS, D), 1.0, 6.0, ((0, 128),))
    norm_gain = jnp.clip(1.0 + 0.18 * jax.random.normal(arg_keys[1], (D,), jnp.float32), 0.1, 1.9)
    expert_ids_keys = jax.random.split(jax.random.fold_in(part_splits[2], 1), TOKENS // TOK_DEV)
    expert_ids_turns = jax.random.permutation(jax.random.fold_in(part_splits[2], 3), TOKENS // TOK_DEV)
    expert_ids = jax.vmap(lambda own, number: routed_block(jax.random.fold_in(part_splits[2], 2), own, number, TOK_DEV, EXPERTS, TOP_K, CAP, 2))(expert_ids_keys, expert_ids_turns).reshape((TOKENS, TOP_K))
    route_weights = jnp.clip(0.1 + 0.79999997 * jax.random.uniform(part_splits[3], (TOKENS, TOP_K), jnp.float32) ** level_of(part_splits[3], (TOKENS, TOP_K), ((0, 128),), -0.2, 0.2), 0.1, 0.9)
    w_gate = noise(arg_keys[4], (D, EXPERTS * FF), D ** -0.5, 0.125, ((1, 128),))
    w_up = noise(arg_keys[5], (D, EXPERTS * FF), D ** -0.5, 0.125, ((1, 128),))
    w_down = noise(arg_keys[6], (EXPERTS * FF, D), FF ** -0.5, 0.09375, ((0, 128),))
    return dict(tokens=tokens, norm_gain=norm_gain, expert_ids=expert_ids, route_weights=route_weights, w_gate=w_gate, w_up=w_up, w_down=w_down)


def reference(tokens, norm_gain, expert_ids, route_weights, w_gate, w_up, w_down):
    values = tokens.astype(jnp.float32)
    scale_rows = lax.rsqrt(lax.optimization_barrier(jnp.mean(values * values, axis=1, keepdims=True)) + 1e-06)
    normed = (values * scale_rows * norm_gain).astype(jnp.bfloat16)
    token_total = tokens.shape[0]
    sources = token_total // TOK_DEV
    per_source = expert_ids.reshape(sources, TOK_DEV * TOP_K)
    onehot = (per_source[:, :, None] == jnp.arange(EXPERTS, dtype=jnp.int32)[None, None, :]).astype(jnp.int32)
    earlier = jnp.cumsum(onehot, axis=1) - onehot
    slot_base = lax.optimization_barrier(jnp.sum(earlier * onehot, axis=2)).reshape(-1).astype(jnp.int32)
    flat_ids = expert_ids.reshape(-1).astype(jnp.int32)
    token_index = (jnp.arange(flat_ids.shape[0], dtype=jnp.int32) // TOP_K).astype(jnp.int32)
    source_index = (token_index // TOK_DEV).astype(jnp.int32)
    slot_index = jnp.remainder(slot_base + source_index, CAP).astype(jnp.int32)
    position = ((flat_ids * sources + source_index) * CAP + slot_index).astype(jnp.int32)
    slot_table = jnp.full((EXPERTS * sources * CAP,), token_total, jnp.int32).at[position].set(token_index)
    slot_table = slot_table.reshape(EXPERTS, sources * CAP)
    padded = jnp.concatenate([normed, jnp.zeros((1, normed.shape[1]), jnp.bfloat16)], axis=0)
    piece_width = FF // (2 * N_TP)

    def one_expert(inputs):
        expert, rows_index = inputs
        in_rows = padded[rows_index]
        first_col = (expert * FF).astype(jnp.int32)
        gate_part = jnp.dot(in_rows, lax.dynamic_slice_in_dim(w_gate, first_col, FF, 1), preferred_element_type=jnp.float32)
        up_part = jnp.dot(in_rows, lax.dynamic_slice_in_dim(w_up, first_col, FF, 1), preferred_element_type=jnp.float32)
        hidden = (jax.nn.silu(gate_part) * up_part).astype(jnp.bfloat16)
        down_rows = lax.dynamic_slice_in_dim(w_down, first_col, FF, 0)
        expert_total = jnp.zeros((in_rows.shape[0], normed.shape[1]), jnp.float32)
        for half_index in range(2):
            half_sum = jnp.zeros((in_rows.shape[0], normed.shape[1]), jnp.float32)
            for core_index in range(N_TP):
                begin = (half_index * N_TP + core_index) * piece_width
                partial_value = jnp.dot(hidden[:, begin:begin + piece_width], down_rows[begin:begin + piece_width], preferred_element_type=jnp.float32)
                half_sum = half_sum + lax.optimization_barrier(partial_value.astype(jnp.bfloat16)).astype(jnp.float32)
            expert_total = expert_total + lax.optimization_barrier(half_sum.astype(jnp.bfloat16)).astype(jnp.float32)
        return lax.optimization_barrier(expert_total.astype(jnp.bfloat16)).astype(jnp.float32)
    results = lax.map(one_expert, (jnp.arange(EXPERTS, dtype=jnp.int32), slot_table))
    picked = results.reshape(-1, normed.shape[1])[position].reshape(token_total, TOP_K, normed.shape[1])
    return lax.optimization_barrier(jnp.sum(picked * route_weights[:, :, None], axis=1)).astype(jnp.bfloat16)
```

```python
import jax
import jax.numpy as jnp
from jax import lax
from jax.experimental import pallas as pl
from jax.experimental.pallas import tpu as pltpu
from jax.sharding import Mesh
from jax.sharding import PartitionSpec as P


ROW = 4
TILE = 128
COLUMNS = 512
SPLIT = 4


def swap(block, axis, mask):
    count = lax.axis_size(axis)
    return lax.ppermute(block, axis, [(i, i ^ mask) for i in range(count)])


def unpack(packed, capacity):
    rows, _, width = packed.shape
    pieces = packed.reshape(rows, SPLIT, capacity, width)
    return pieces.transpose(0, 2, 1, 3).reshape(rows * capacity, SPLIT * width)


def pack(block, rows):
    capacity, width = block.shape[0] // rows, block.shape[1] // SPLIT
    pieces = block.reshape(rows, capacity, SPLIT, width)
    return pieces.transpose(0, 2, 1, 3).reshape(rows, SPLIT * capacity, width)


def along_z(packed):
    return lax.all_to_all(packed, "z", split_axis=0, concat_axis=0, tiled=True)


def add(a, b):
    return (a.astype(jnp.float32) + b.astype(jnp.float32)).astype(jnp.bfloat16)


def expert_kernel(mine, other, w_gate, w_up, w_down, out_mine, out_other, rows, hidden, down, sem):
    step, steps = pl.program_id(0), pl.num_programs(0)
    count, tile = mine.shape[0], w_gate.shape[1]
    load = pltpu.make_async_copy(w_down, down, sem)

    @pl.when(step == 0)
    def _():
        load.start()
        rows[:count] = mine[...]
        rows[count:] = other[...]

    both = jnp.dot(
        rows[...],
        jnp.concatenate([w_gate[...], w_up[...]], axis=1),
        preferred_element_type=jnp.float32,
    )
    gate, up = both[:, :tile], both[:, tile:]
    hidden[step] = (gate / (1.0 + jnp.exp(-gate)) * up).astype(jnp.bfloat16)

    @pl.when(step == steps - 1)
    def _():
        load.wait()
        units = jnp.concatenate([hidden[i] for i in range(hidden.shape[0])], axis=1)
        for first in range(0, down.shape[1], COLUMNS):
            part = jnp.dot(
                units, down[:, first : first + COLUMNS], preferred_element_type=jnp.float32
            ).astype(jnp.bfloat16)
            out_mine[:, first : first + COLUMNS] = part[:count]
            out_other[:, first : first + COLUMNS] = part[count:]


def expert(mine, other, w_gate, w_up, w_down):
    count, model_width = mine.shape
    units = w_gate.shape[1]
    steps = units // TILE
    whole = pl.BlockSpec((count, model_width), lambda i: (0, 0))
    columns = pl.BlockSpec((model_width, TILE), lambda i: (0, i))
    out = jax.ShapeDtypeStruct((count, model_width), jnp.bfloat16)
    return pl.pallas_call(
        expert_kernel,
        grid=(steps,),
        in_specs=[whole, whole, columns, columns, pl.BlockSpec(memory_space=pl.ANY)],
        out_specs=[whole, whole],
        out_shape=[out, out],
        scratch_shapes=[
            pltpu.VMEM((2 * count, model_width), jnp.bfloat16),
            pltpu.VMEM((steps, 2 * count, TILE), jnp.bfloat16),
            pltpu.VMEM((units, model_width), jnp.bfloat16),
            pltpu.SemaphoreType.DMA,
        ],
        compiler_params=pltpu.CompilerParams(vmem_limit_bytes=40 * 2**20),
        cost_estimate=pl.CostEstimate(
            flops=12 * count * model_width * units,
            bytes_accessed=6 * model_width * units + 8 * count * model_width,
            transcendentals=2 * count * units,
        ),
    )(mine, other, w_gate, w_up, w_down)


def to_halves(packed, weights, capacity):
    rows = unpack(packed, capacity)
    theirs = swap(rows, "x", 1)
    mine = jnp.concatenate([rows, theirs], axis=0)
    other = swap(mine, "tp", 1)
    out_mine, out_other = expert(mine, other, *weights)
    return add(out_mine, swap(out_other, "tp", 1))


def to_outputs(half, nz):
    count = half.shape[0] // 2
    theirs = swap(half[count:], "x", 1)
    return pack(add(half[:count], theirs), nz)


def local(tokens, norm_gain, expert_ids, route_weights, w_gate, w_up, w_down):
    nz = lax.axis_size("z")
    expert_count = nz * ROW // 2
    tok_count, model_width = tokens.shape
    top_count = expert_ids.shape[1]
    capacity = 2 * max(1, 5 * tok_count * top_count // (8 * expert_count))
    width = model_width // SPLIT
    weights = (w_gate, w_up, w_down)
    pair = lax.axis_index("x") // 2

    values = tokens.astype(jnp.float32)
    scale_rows = lax.rsqrt(jnp.mean(values * values, axis=1, keepdims=True) + 1e-06)
    normed = (values * scale_rows * norm_gain).astype(jnp.bfloat16)
    stacked = jnp.concatenate(
        [normed[:, q * width : (q + 1) * width] for q in range(SPLIT)], axis=0
    )

    before = jnp.arange(tok_count)[:, None] > jnp.arange(tok_count)[None, :]
    places, parts = [], []
    for k in range(top_count):
        mine = expert_ids[:, k]
        same = sum((mine[:, None] == expert_ids[:, j][None, :]).astype(jnp.int32) for j in range(top_count))
        rank = jnp.sum(jnp.where(before, same, 0), axis=1)
        places.append((mine // 2) * capacity + rank)
        parts.append((mine % 2) ^ pair)

    line = jnp.arange(nz * SPLIT * capacity, dtype=jnp.int32)
    line_piece = (line // capacity) % SPLIT
    line_place = (line // (SPLIT * capacity)) * capacity + line % capacity
    piece = jnp.repeat(jnp.arange(SPLIT, dtype=jnp.int32), tok_count)

    def chosen(part, k):
        place = jnp.tile(jnp.where(parts[k] == part, places[k], -1), SPLIT)
        return (line_piece[:, None] == piece[None, :]) & (line_place[:, None] == place[None, :])

    def outgoing(part):
        select = chosen(part, 0)
        for k in range(1, top_count):
            select = select | chosen(part, k)
        message = jnp.dot(select.astype(jnp.bfloat16), stacked, preferred_element_type=jnp.float32)
        return message.astype(jnp.bfloat16).reshape(nz, SPLIT * capacity, width)

    near = along_z(outgoing(0))
    crossed = swap(outgoing(1), "x", 3)
    near, crossed = lax.optimization_barrier((near, crossed))
    far = along_z(crossed)
    near_half = to_halves(near, weights, capacity)
    far, near_half = lax.optimization_barrier((far, near_half))
    near_out = to_outputs(near_half, nz)
    near_back = along_z(near_out)
    far_out = to_outputs(to_halves(far, weights, capacity), nz)
    near_back, far_out = lax.optimization_barrier((near_back, far_out))
    far_back = along_z(far_out)
    far_back = swap(far_back, "x", 3)

    mixed = jnp.zeros((SPLIT * tok_count, width), jnp.float32)
    for k in range(top_count):
        picked = jnp.zeros((SPLIT * tok_count, width), jnp.float32)
        for part, back in ((0, near_back), (1, far_back)):
            select = chosen(part, k).T.astype(jnp.bfloat16)
            picked = picked + jnp.dot(
                select, back.reshape(-1, width), preferred_element_type=jnp.float32
            )
        mixed = mixed + picked * jnp.tile(route_weights[:, k], SPLIT)[:, None]
    mixed = mixed.astype(jnp.bfloat16)
    return jnp.concatenate(
        [mixed[q * tok_count : (q + 1) * tok_count] for q in range(SPLIT)], axis=1
    )


def solution(mesh):
    groups, ep, cores = (mesh.shape[name] for name in ("grp", "ep", "tp"))
    grid = Mesh(mesh.devices.reshape(groups, ep // ROW, ROW, cores), ("grp", "z", "x", "tp"))
    tok = P(("grp", "z", "x", "tp"), None)
    placed = (
        tok,
        P(),
        tok,
        tok,
        P(None, ("z", "x", "tp")),
        P(None, ("z", "x", "tp")),
        P(("z", "x", "tp"), None),
    )

    return jax.shard_map(local, mesh=grid, in_specs=placed, out_specs=tok, check_vma=False)
```

```python
import jax
import jax.numpy as jnp
from jax import lax
from jax.experimental import pallas as pl
from jax.experimental.pallas import tpu as pltpu
from jax.sharding import Mesh
from jax.sharding import PartitionSpec as P


ROW = 4
TILE = 128
COLUMNS = 512
SPLIT = 4


def swap(block, axis, mask):
    count = lax.axis_size(axis)
    return lax.ppermute(block, axis, [(i, i ^ mask) for i in range(count)])


def unpack(packed, capacity):
    rows, _, width = packed.shape
    pieces = packed.reshape(rows, SPLIT, capacity, width)
    return pieces.transpose(0, 2, 1, 3).reshape(rows * capacity, SPLIT * width)


def along_z(packed):
    return lax.all_to_all(packed, "z", split_axis=0, concat_axis=0, tiled=True)


def add(a, b):
    return (a.astype(jnp.float32) + b.astype(jnp.float32)).astype(jnp.bfloat16)


def expert_kernel(mine, other, w_gate, w_up, w_down, out_mine, out_other, rows, hidden, down, sem):
    step, steps = pl.program_id(0), pl.num_programs(0)
    count, tile = mine.shape[0], w_gate.shape[1]
    load = pltpu.make_async_copy(w_down, down, sem)

    @pl.when(step == 0)
    def _():
        load.start()
        rows[:count] = mine[...]
        rows[count:] = other[...]

    both = jnp.dot(
        rows[...],
        jnp.concatenate([w_gate[...], w_up[...]], axis=1),
        preferred_element_type=jnp.float32,
    )
    gate, up = both[:, :tile], both[:, tile:]
    hidden[step] = (gate / (1.0 + jnp.exp(-gate)) * up).astype(jnp.bfloat16)

    @pl.when(step == steps - 1)
    def _():
        load.wait()
        units = jnp.concatenate([hidden[i] for i in range(hidden.shape[0])], axis=1)
        for first in range(0, down.shape[1], COLUMNS):
            part = jnp.dot(
                units, down[:, first : first + COLUMNS], preferred_element_type=jnp.float32
            ).astype(jnp.bfloat16)
            out_mine[:, first : first + COLUMNS] = part[:count]
            out_other[:, first : first + COLUMNS] = part[count:]


def expert(mine, other, w_gate, w_up, w_down):
    count, model_width = mine.shape
    units = w_gate.shape[1]
    steps = units // TILE
    whole = pl.BlockSpec((count, model_width), lambda i: (0, 0))
    columns = pl.BlockSpec((model_width, TILE), lambda i: (0, i))
    out = jax.ShapeDtypeStruct((count, model_width), jnp.bfloat16)
    return pl.pallas_call(
        expert_kernel,
        grid=(steps,),
        in_specs=[whole, whole, columns, columns, pl.BlockSpec(memory_space=pl.ANY)],
        out_specs=[whole, whole],
        out_shape=[out, out],
        scratch_shapes=[
            pltpu.VMEM((2 * count, model_width), jnp.bfloat16),
            pltpu.VMEM((steps, 2 * count, TILE), jnp.bfloat16),
            pltpu.VMEM((units, model_width), jnp.bfloat16),
            pltpu.SemaphoreType.DMA,
        ],
        compiler_params=pltpu.CompilerParams(vmem_limit_bytes=50 * 2**20),
        cost_estimate=pl.CostEstimate(
            flops=12 * count * model_width * units,
            bytes_accessed=6 * model_width * units + 8 * count * model_width,
            transcendentals=2 * count * units,
        ),
    )(mine, other, w_gate, w_up, w_down)


def merge_kernel(own, theirs, order, out):
    total = (own[...].astype(jnp.float32) + theirs[...].astype(jnp.float32)).astype(jnp.bfloat16)
    width = out.shape[1]
    stacked = jnp.concatenate(
        [total[:, first : first + width] for first in range(0, total.shape[1], width)], axis=0
    )
    out[...] = jnp.dot(order[...], stacked, preferred_element_type=jnp.float32).astype(jnp.bfloat16)


def merge(own, theirs, order, nz):
    count, model_width = own.shape
    width = model_width // SPLIT
    packed = pl.pallas_call(
        merge_kernel,
        out_shape=jax.ShapeDtypeStruct((count * SPLIT, width), jnp.bfloat16),
        in_specs=[pl.BlockSpec(memory_space=pltpu.VMEM)] * 3,
        out_specs=pl.BlockSpec(memory_space=pltpu.VMEM),
        compiler_params=pltpu.CompilerParams(vmem_limit_bytes=12 * 2**20),
        cost_estimate=pl.CostEstimate(
            flops=2 * (count * SPLIT) ** 2 * width, bytes_accessed=8 * count * model_width, transcendentals=0
        ),
    )(own, theirs, order)
    return packed.reshape(nz, -1, width)


def core_sums(rows, weights):
    other = swap(rows, "tp", 1)
    out_mine, out_other = expert(rows, other, *weights)
    return add(out_mine, swap(out_other, "tp", 1))


def local(tokens, norm_gain, expert_ids, route_weights, w_gate, w_up, w_down):
    nz = lax.axis_size("z")
    expert_count = nz * ROW // 2
    tok_count, model_width = tokens.shape
    top_count = expert_ids.shape[1]
    capacity = 2 * max(1, 5 * tok_count * top_count // (8 * expert_count))
    width = model_width // SPLIT
    weights = (w_gate, w_up, w_down)
    pair = lax.axis_index("x") // 2

    values = tokens.astype(jnp.float32)
    scale_rows = lax.rsqrt(jnp.mean(values * values, axis=1, keepdims=True) + 1e-06)
    normed = (values * scale_rows * norm_gain).astype(jnp.bfloat16)
    stacked = jnp.concatenate(
        [normed[:, q * width : (q + 1) * width] for q in range(SPLIT)], axis=0
    )

    before = jnp.arange(tok_count)[:, None] > jnp.arange(tok_count)[None, :]
    places, parts = [], []
    for k in range(top_count):
        mine = expert_ids[:, k]
        same = sum((mine[:, None] == expert_ids[:, j][None, :]).astype(jnp.int32) for j in range(top_count))
        rank = jnp.sum(jnp.where(before, same, 0), axis=1)
        places.append((mine // 2) * capacity + rank)
        parts.append((mine % 2) ^ pair)

    line = jnp.arange(nz * SPLIT * capacity, dtype=jnp.int32)
    line_piece = (line // capacity) % SPLIT
    line_place = (line // (SPLIT * capacity)) * capacity + line % capacity
    piece = jnp.repeat(jnp.arange(SPLIT, dtype=jnp.int32), tok_count)

    def chosen(part, k):
        place = jnp.tile(jnp.where(parts[k] == part, places[k], -1), SPLIT)
        return (line_piece[:, None] == piece[None, :]) & (line_place[:, None] == place[None, :])

    def outgoing(part):
        select = chosen(part, 0)
        for k in range(1, top_count):
            select = select | chosen(part, k)
        message = jnp.dot(select.astype(jnp.bfloat16), stacked, preferred_element_type=jnp.float32)
        return message.astype(jnp.bfloat16).reshape(nz, SPLIT * capacity, width)

    stacked_piece = jnp.repeat(jnp.arange(SPLIT, dtype=jnp.int32), nz * capacity)
    stacked_place = jnp.tile(jnp.arange(nz * capacity, dtype=jnp.int32), SPLIT)
    order = (
        (line_piece[:, None] == stacked_piece[None, :]) & (line_place[:, None] == stacked_place[None, :])
    ).astype(jnp.bfloat16)

    near = along_z(outgoing(0))
    crossed = swap(outgoing(1), "x", 3)
    near, crossed, order = lax.optimization_barrier((near, crossed, order))
    far = along_z(crossed)

    rows = unpack(near, capacity)
    theirs = swap(rows, "x", 1)
    own_half = core_sums(rows, weights)
    their_half = core_sums(theirs, weights)
    theirs = swap(their_half, "x", 1)
    near_out = merge(own_half, theirs, order, nz)
    far, near_out = lax.optimization_barrier((far, near_out))
    near_back = along_z(near_out)

    rows = unpack(far, capacity)
    theirs = swap(rows, "x", 1)
    own_half = core_sums(rows, weights)
    their_half = core_sums(theirs, weights)
    theirs = swap(their_half, "x", 1)
    far_out = merge(own_half, theirs, order, nz)
    near_back, far_out = lax.optimization_barrier((near_back, far_out))
    far_back = along_z(far_out)
    far_back = swap(far_back, "x", 3)

    mixed = jnp.zeros((SPLIT * tok_count, width), jnp.float32)
    for k in range(top_count):
        picked = jnp.zeros((SPLIT * tok_count, width), jnp.float32)
        for part, back in ((0, near_back), (1, far_back)):
            select = chosen(part, k).T.astype(jnp.bfloat16)
            picked = picked + jnp.dot(
                select, back.reshape(-1, width), preferred_element_type=jnp.float32
            )
        mixed = mixed + picked * jnp.tile(route_weights[:, k], SPLIT)[:, None]
    mixed = mixed.astype(jnp.bfloat16)
    return jnp.concatenate(
        [mixed[q * tok_count : (q + 1) * tok_count] for q in range(SPLIT)], axis=1
    )


def solution(mesh):
    groups, ep, cores = (mesh.shape[name] for name in ("grp", "ep", "tp"))
    grid = Mesh(mesh.devices.reshape(groups, ep // ROW, ROW, cores), ("grp", "z", "x", "tp"))
    tok = P(("grp", "z", "x", "tp"), None)
    placed = (
        tok,
        P(),
        tok,
        tok,
        P(None, ("z", "x", "tp")),
        P(None, ("z", "x", "tp")),
        P(("z", "x", "tp"), None),
    )

    return jax.shard_map(local, mesh=grid, in_specs=placed, out_specs=tok, check_vma=False)
```

```python
import jax
import jax.numpy as jnp
from jax import lax
from jax.experimental import pallas as pl
from jax.experimental.pallas import tpu as pltpu
from jax.sharding import Mesh
from jax.sharding import PartitionSpec as P


ROW = 4
TILE = 128
FFN_LIMIT = 20
COLUMNS = 256
SPLIT = 4


def swap(block, axis, mask):
    count = lax.axis_size(axis)
    return lax.ppermute(block, axis, [(i, i ^ mask) for i in range(count)])


def unpack(packed, capacity):
    rows, _, width = packed.shape
    pieces = packed.reshape(rows, SPLIT, capacity, width)
    return pieces.transpose(0, 2, 1, 3).reshape(rows * capacity, SPLIT * width)


def along_z(packed):
    return lax.all_to_all(packed, "z", split_axis=0, concat_axis=0, tiled=True)


def add(a, b):
    return (a.astype(jnp.float32) + b.astype(jnp.float32)).astype(jnp.bfloat16)


def expert_kernel(mine, other, w_gate, w_up, w_down, out_mine, out_other, hidden):
    count, model_width = mine.shape
    units = w_gate.shape[1]

    def gated(i, carry):
        tile = pl.ds(pl.multiple_of(i * TILE, TILE), TILE)
        both = jnp.dot(
            jnp.concatenate([mine[...], other[...]], axis=0),
            jnp.concatenate([w_gate[:, tile], w_up[:, tile]], axis=1),
            preferred_element_type=jnp.float32,
        )
        gate, up = both[:, :TILE], both[:, TILE:]
        hidden[:, tile] = (gate / (1.0 + jnp.exp(-gate)) * up).astype(jnp.bfloat16)
        return carry

    lax.fori_loop(0, units // TILE, gated, 0)

    def down(i, carry):
        tile = pl.ds(pl.multiple_of(i * COLUMNS, COLUMNS), COLUMNS)
        part = jnp.dot(hidden[...], w_down[:, tile], preferred_element_type=jnp.float32)
        out_mine[:, tile] = part[:count].astype(jnp.bfloat16)
        out_other[:, tile] = part[count:].astype(jnp.bfloat16)
        return carry

    lax.fori_loop(0, model_width // COLUMNS, down, 0)


def expert(mine, other, w_gate, w_up, w_down):
    count, model_width = mine.shape
    units = w_gate.shape[1]
    vmem = pl.BlockSpec(memory_space=pltpu.VMEM)
    out = jax.ShapeDtypeStruct((count, model_width), jnp.bfloat16)
    return pl.pallas_call(
        expert_kernel,
        in_specs=[vmem] * 5,
        out_specs=[vmem, vmem],
        out_shape=[out, out],
        scratch_shapes=[pltpu.VMEM((2 * count, units), jnp.bfloat16)],
        compiler_params=pltpu.CompilerParams(vmem_limit_bytes=FFN_LIMIT * 2**20),
        cost_estimate=pl.CostEstimate(
            flops=12 * count * model_width * units,
            bytes_accessed=8 * count * model_width,
            transcendentals=2 * count * units,
        ),
    )(mine, other, w_gate, w_up, w_down)


def merge_kernel(own, theirs, order, out):
    total = (own[...].astype(jnp.float32) + theirs[...].astype(jnp.float32)).astype(jnp.bfloat16)
    width = out.shape[1]
    stacked = jnp.concatenate(
        [total[:, first : first + width] for first in range(0, total.shape[1], width)], axis=0
    )
    out[...] = jnp.dot(order[...], stacked, preferred_element_type=jnp.float32).astype(jnp.bfloat16)


def merge(own, theirs, order, nz):
    count, model_width = own.shape
    width = model_width // SPLIT
    packed = pl.pallas_call(
        merge_kernel,
        out_shape=jax.ShapeDtypeStruct((count * SPLIT, width), jnp.bfloat16),
        in_specs=[pl.BlockSpec(memory_space=pltpu.VMEM)] * 3,
        out_specs=pl.BlockSpec(memory_space=pltpu.VMEM),
        compiler_params=pltpu.CompilerParams(vmem_limit_bytes=12 * 2**20),
        cost_estimate=pl.CostEstimate(
            flops=2 * (count * SPLIT) ** 2 * width, bytes_accessed=8 * count * model_width, transcendentals=0
        ),
    )(own, theirs, order)
    return packed.reshape(nz, -1, width)


def core_sums(rows, weights):
    other = swap(rows, "tp", 1)
    out_mine, out_other = expert(rows, other, *weights)
    return add(out_mine, swap(out_other, "tp", 1))


def local(tokens, norm_gain, expert_ids, route_weights, w_gate, w_up, w_down):
    nz = lax.axis_size("z")
    expert_count = nz * ROW // 2
    tok_count, model_width = tokens.shape
    top_count = expert_ids.shape[1]
    capacity = 2 * max(1, 5 * tok_count * top_count // (8 * expert_count))
    width = model_width // SPLIT
    weights = (w_gate, w_up, w_down)
    pair = lax.axis_index("x") // 2

    values = tokens.astype(jnp.float32)
    scale_rows = lax.rsqrt(jnp.mean(values * values, axis=1, keepdims=True) + 1e-06)
    normed = (values * scale_rows * norm_gain).astype(jnp.bfloat16)
    stacked = jnp.concatenate(
        [normed[:, q * width : (q + 1) * width] for q in range(SPLIT)], axis=0
    )

    before = jnp.arange(tok_count)[:, None] > jnp.arange(tok_count)[None, :]
    places, parts = [], []
    for k in range(top_count):
        mine = expert_ids[:, k]
        same = sum((mine[:, None] == expert_ids[:, j][None, :]).astype(jnp.int32) for j in range(top_count))
        rank = jnp.sum(jnp.where(before, same, 0), axis=1)
        places.append((mine // 2) * capacity + rank)
        parts.append((mine % 2) ^ pair)

    line = jnp.arange(nz * SPLIT * capacity, dtype=jnp.int32)
    line_piece = (line // capacity) % SPLIT
    line_place = (line // (SPLIT * capacity)) * capacity + line % capacity
    piece = jnp.repeat(jnp.arange(SPLIT, dtype=jnp.int32), tok_count)

    def chosen(part, k):
        place = jnp.tile(jnp.where(parts[k] == part, places[k], -1), SPLIT)
        return (line_piece[:, None] == piece[None, :]) & (line_place[:, None] == place[None, :])

    def outgoing(part):
        select = chosen(part, 0)
        for k in range(1, top_count):
            select = select | chosen(part, k)
        message = jnp.dot(select.astype(jnp.bfloat16), stacked, preferred_element_type=jnp.float32)
        return message.astype(jnp.bfloat16).reshape(nz, SPLIT * capacity, width)

    stacked_piece = jnp.repeat(jnp.arange(SPLIT, dtype=jnp.int32), nz * capacity)
    stacked_place = jnp.tile(jnp.arange(nz * capacity, dtype=jnp.int32), SPLIT)
    order = (
        (line_piece[:, None] == stacked_piece[None, :]) & (line_place[:, None] == stacked_place[None, :])
    ).astype(jnp.bfloat16)

    near = along_z(outgoing(0))
    crossed = swap(outgoing(1), "x", 3)
    near, crossed, order = lax.optimization_barrier((near, crossed, order))
    far = along_z(crossed)

    rows = unpack(near, capacity)
    theirs = swap(rows, "x", 1)
    own_half = core_sums(rows, weights)
    their_half = core_sums(theirs, weights)
    theirs = swap(their_half, "x", 1)
    near_out = merge(own_half, theirs, order, nz)
    far, near_out = lax.optimization_barrier((far, near_out))
    near_back = along_z(near_out)

    rows = unpack(far, capacity)
    theirs = swap(rows, "x", 1)
    own_half = core_sums(rows, weights)
    their_half = core_sums(theirs, weights)
    theirs = swap(their_half, "x", 1)
    far_out = merge(own_half, theirs, order, nz)
    near_back, far_out = lax.optimization_barrier((near_back, far_out))
    far_back = along_z(far_out)
    far_back = swap(far_back, "x", 3)

    mixed = jnp.zeros((SPLIT * tok_count, width), jnp.float32)
    for k in range(top_count):
        picked = jnp.zeros((SPLIT * tok_count, width), jnp.float32)
        for part, back in ((0, near_back), (1, far_back)):
            select = chosen(part, k).T.astype(jnp.bfloat16)
            picked = picked + jnp.dot(
                select, back.reshape(-1, width), preferred_element_type=jnp.float32
            )
        mixed = mixed + picked * jnp.tile(route_weights[:, k], SPLIT)[:, None]
    mixed = mixed.astype(jnp.bfloat16)
    return jnp.concatenate(
        [mixed[q * tok_count : (q + 1) * tok_count] for q in range(SPLIT)], axis=1
    )


def solution(mesh):
    groups, ep, cores = (mesh.shape[name] for name in ("grp", "ep", "tp"))
    grid = Mesh(mesh.devices.reshape(groups, ep // ROW, ROW, cores), ("grp", "z", "x", "tp"))
    tok = P(("grp", "z", "x", "tp"), None)
    placed = (
        tok,
        P(),
        tok,
        tok,
        P(None, ("z", "x", "tp")),
        P(None, ("z", "x", "tp")),
        P(("z", "x", "tp"), None),
    )

    return jax.shard_map(local, mesh=grid, in_specs=placed, out_specs=tok, check_vma=False)
```

```python
import jax
import jax.numpy as jnp
from jax import lax
from jax.experimental import pallas as pl
from jax.experimental.pallas import tpu as pltpu
from jax.sharding import Mesh
from jax.sharding import PartitionSpec as P


ROW = 4
TILE = 128
FFN_LIMIT = 50
COLUMNS = 512
SPLIT = 4


def swap(block, axis, mask):
    count = lax.axis_size(axis)
    return lax.ppermute(block, axis, [(i, i ^ mask) for i in range(count)])


def unpack(packed, capacity):
    rows, _, width = packed.shape
    pieces = packed.reshape(rows, SPLIT, capacity, width)
    return pieces.transpose(0, 2, 1, 3).reshape(rows * capacity, SPLIT * width)


def along_z(packed):
    return lax.all_to_all(packed, "z", split_axis=0, concat_axis=0, tiled=True)


def add(a, b):
    return (a.astype(jnp.float32) + b.astype(jnp.float32)).astype(jnp.bfloat16)


def expert_kernel(*refs):
    ins, (w_gate, w_up, w_down), outs = refs[:4], refs[4:7], refs[7:11]
    rows, hidden, down, sem = refs[11:]
    step, steps = pl.program_id(0), pl.num_programs(0)
    count, tile = ins[0].shape[0], w_gate.shape[1]
    load = pltpu.make_async_copy(w_down, down, sem)

    @pl.when(step == 0)
    def _():
        load.start()
        for i, source in enumerate(ins):
            rows[i * count : (i + 1) * count] = source[...]

    both = jnp.dot(
        rows[...],
        jnp.concatenate([w_gate[...], w_up[...]], axis=1),
        preferred_element_type=jnp.float32,
    )
    gate, up = both[:, :tile], both[:, tile:]
    hidden[step] = (gate / (1.0 + jnp.exp(-gate)) * up).astype(jnp.bfloat16)

    @pl.when(step == steps - 1)
    def _():
        load.wait()
        units = jnp.concatenate([hidden[i] for i in range(hidden.shape[0])], axis=1)
        for first in range(0, down.shape[1], COLUMNS):
            part = jnp.dot(
                units, down[:, first : first + COLUMNS], preferred_element_type=jnp.float32
            ).astype(jnp.bfloat16)
            for i, target in enumerate(outs):
                target[:, first : first + COLUMNS] = part[i * count : (i + 1) * count]


def expert(blocks, w_gate, w_up, w_down):
    count, model_width = blocks[0].shape
    units = w_gate.shape[1]
    steps = units // TILE
    total = len(blocks) * count
    whole = pl.BlockSpec((count, model_width), lambda i: (0, 0))
    columns = pl.BlockSpec((model_width, TILE), lambda i: (0, i))
    out = jax.ShapeDtypeStruct((count, model_width), jnp.bfloat16)
    return pl.pallas_call(
        expert_kernel,
        grid=(steps,),
        in_specs=[whole] * 4 + [columns, columns, pl.BlockSpec(memory_space=pl.ANY)],
        out_specs=[whole] * 4,
        out_shape=[out] * 4,
        scratch_shapes=[
            pltpu.VMEM((total, model_width), jnp.bfloat16),
            pltpu.VMEM((steps, total, TILE), jnp.bfloat16),
            pltpu.VMEM((units, model_width), jnp.bfloat16),
            pltpu.SemaphoreType.DMA,
        ],
        compiler_params=pltpu.CompilerParams(vmem_limit_bytes=FFN_LIMIT * 2**20),
        cost_estimate=pl.CostEstimate(
            flops=6 * total * model_width * units,
            bytes_accessed=6 * model_width * units + 4 * total * model_width,
            transcendentals=total * units,
        ),
    )(*blocks, w_gate, w_up, w_down)


def merge_kernel(*refs):
    parts, order, out = refs[:-2], refs[-2], refs[-1]
    half = len(parts) // 2
    width = out.shape[1]
    own, theirs = (
        jnp.concatenate([part[...] for part in some], axis=0).astype(jnp.float32)
        for some in (parts[:half], parts[half:])
    )
    total = (own + theirs).astype(jnp.bfloat16)
    stacked = jnp.concatenate(
        [total[:, first : first + width] for first in range(0, total.shape[1], width)], axis=0
    )
    out[...] = jnp.dot(order[...], stacked, preferred_element_type=jnp.float32).astype(jnp.bfloat16)


def merge(own, theirs, order, nz):
    count = sum(part.shape[0] for part in own)
    model_width = own[0].shape[1]
    width = model_width // SPLIT
    vmem = pl.BlockSpec(memory_space=pltpu.VMEM)
    packed = pl.pallas_call(
        merge_kernel,
        out_shape=jax.ShapeDtypeStruct((count * SPLIT, width), jnp.bfloat16),
        in_specs=[vmem] * (2 * len(own) + 1),
        out_specs=vmem,
        compiler_params=pltpu.CompilerParams(vmem_limit_bytes=12 * 2**20),
        cost_estimate=pl.CostEstimate(
            flops=2 * (count * SPLIT) ** 2 * width, bytes_accessed=8 * count * model_width, transcendentals=0
        ),
    )(*own, *theirs, order)
    return packed.reshape(nz, -1, width)


def through_row(packed, weights, capacity, pieces):
    rows = unpack(packed, capacity)
    size = rows.shape[0] // pieces
    cut = [rows[i * size : (i + 1) * size] for i in range(pieces)]
    own, theirs = [], []
    for mine in cut:
        partner = swap(mine, "x", 1)
        mine_other = swap(mine, "tp", 1)
        partner_other = swap(partner, "tp", 1)
        sums = expert((mine, partner, mine_other, partner_other), *weights)
        partner_half = add(sums[1], swap(sums[3], "tp", 1))
        own.append(add(sums[0], swap(sums[2], "tp", 1)))
        theirs.append(swap(partner_half, "x", 1))
    return own, theirs


def local(tokens, norm_gain, expert_ids, route_weights, w_gate, w_up, w_down):
    nz = lax.axis_size("z")
    expert_count = nz * ROW // 2
    tok_count, model_width = tokens.shape
    top_count = expert_ids.shape[1]
    capacity = 2 * max(1, 5 * tok_count * top_count // (8 * expert_count))
    width = model_width // SPLIT
    weights = (w_gate, w_up, w_down)
    pair = lax.axis_index("x") // 2

    values = tokens.astype(jnp.float32)
    scale_rows = lax.rsqrt(jnp.mean(values * values, axis=1, keepdims=True) + 1e-06)
    normed = (values * scale_rows * norm_gain).astype(jnp.bfloat16)
    stacked = jnp.concatenate(
        [normed[:, q * width : (q + 1) * width] for q in range(SPLIT)], axis=0
    )

    before = jnp.arange(tok_count)[:, None] > jnp.arange(tok_count)[None, :]
    places, parts = [], []
    for k in range(top_count):
        mine = expert_ids[:, k]
        same = sum((mine[:, None] == expert_ids[:, j][None, :]).astype(jnp.int32) for j in range(top_count))
        rank = jnp.sum(jnp.where(before, same, 0), axis=1)
        places.append((mine // 2) * capacity + rank)
        parts.append((mine % 2) ^ pair)

    line = jnp.arange(nz * SPLIT * capacity, dtype=jnp.int32)
    line_piece = (line // capacity) % SPLIT
    line_place = (line // (SPLIT * capacity)) * capacity + line % capacity
    piece = jnp.repeat(jnp.arange(SPLIT, dtype=jnp.int32), tok_count)

    def chosen(part, k):
        place = jnp.tile(jnp.where(parts[k] == part, places[k], -1), SPLIT)
        return (line_piece[:, None] == piece[None, :]) & (line_place[:, None] == place[None, :])

    def outgoing(part):
        select = chosen(part, 0)
        for k in range(1, top_count):
            select = select | chosen(part, k)
        message = jnp.dot(select.astype(jnp.bfloat16), stacked, preferred_element_type=jnp.float32)
        return message.astype(jnp.bfloat16).reshape(nz, SPLIT * capacity, width)

    stacked_piece = jnp.repeat(jnp.arange(SPLIT, dtype=jnp.int32), nz * capacity)
    stacked_place = jnp.tile(jnp.arange(nz * capacity, dtype=jnp.int32), SPLIT)
    order = (
        (line_piece[:, None] == stacked_piece[None, :]) & (line_place[:, None] == stacked_place[None, :])
    ).astype(jnp.bfloat16)

    near = along_z(outgoing(0))
    crossed = swap(outgoing(1), "x", 3)
    near, crossed, order = lax.optimization_barrier((near, crossed, order))
    far = along_z(crossed)

    own, theirs = through_row(near, weights, capacity, 2)
    near_out = merge(own, theirs, order, nz)
    far, near_out = lax.optimization_barrier((far, near_out))
    near_back = along_z(near_out)
    own, theirs = through_row(far, weights, capacity, 1)
    far_out = merge(own, theirs, order, nz)
    near_back, far_out = lax.optimization_barrier((near_back, far_out))
    far_back = along_z(far_out)
    far_back = swap(far_back, "x", 3)

    mixed = jnp.zeros((SPLIT * tok_count, width), jnp.float32)
    for k in range(top_count):
        picked = jnp.zeros((SPLIT * tok_count, width), jnp.float32)
        for part, back in ((0, near_back), (1, far_back)):
            select = chosen(part, k).T.astype(jnp.bfloat16)
            picked = picked + jnp.dot(
                select, back.reshape(-1, width), preferred_element_type=jnp.float32
            )
        mixed = mixed + picked * jnp.tile(route_weights[:, k], SPLIT)[:, None]
    mixed = mixed.astype(jnp.bfloat16)
    return jnp.concatenate(
        [mixed[q * tok_count : (q + 1) * tok_count] for q in range(SPLIT)], axis=1
    )


def solution(mesh):
    groups, ep, cores = (mesh.shape[name] for name in ("grp", "ep", "tp"))
    grid = Mesh(mesh.devices.reshape(groups, ep // ROW, ROW, cores), ("grp", "z", "x", "tp"))
    tok = P(("grp", "z", "x", "tp"), None)
    placed = (
        tok,
        P(),
        tok,
        tok,
        P(None, ("z", "x", "tp")),
        P(None, ("z", "x", "tp")),
        P(("z", "x", "tp"), None),
    )

    return jax.shard_map(local, mesh=grid, in_specs=placed, out_specs=tok, check_vma=False)
```

```python
import jax
import jax.numpy as jnp
from jax import lax
from jax.experimental import pallas as pl
from jax.experimental.pallas import tpu as pltpu
from jax.sharding import Mesh
from jax.sharding import PartitionSpec as P


ROW = 4
DEPTH = 512
GATED = 32
FFN_LIMIT = 50
COLUMNS = 1024
SPLIT = 4


def swap(block, axis, mask):
    count = lax.axis_size(axis)
    return lax.ppermute(block, axis, [(i, i ^ mask) for i in range(count)])


def unpack(packed, capacity):
    rows, _, width = packed.shape
    pieces = packed.reshape(rows, SPLIT, capacity, width)
    return pieces.transpose(0, 2, 1, 3).reshape(rows * capacity, SPLIT * width)


def along_z(packed):
    return lax.all_to_all(packed, "z", split_axis=0, concat_axis=0, tiled=True)


def add(a, b):
    return (a.astype(jnp.float32) + b.astype(jnp.float32)).astype(jnp.bfloat16)


def expert_kernel(*refs):
    ins, (w_gate, w_up, w_down), outs = refs[:4], refs[4:7], refs[7:11]
    rows, sums, hidden, down, sem = refs[11:]
    step, steps = pl.program_id(0), pl.num_programs(0)
    count, (depth, units) = ins[0].shape[0], w_gate.shape
    load = pltpu.make_async_copy(w_down, down, sem)

    @pl.when(step == 0)
    def _():
        load.start()
        for i, source in enumerate(ins):
            rows[i * count : (i + 1) * count] = source[...]
        sums[...] = jnp.zeros_like(sums)

    sums[...] += jnp.dot(
        rows[:, pl.ds(pl.multiple_of(step * depth, depth), depth)],
        jnp.concatenate([w_gate[...], w_up[...]], axis=1),
        preferred_element_type=jnp.float32,
    )

    @pl.when(step == steps - 1)
    def _():
        def gated(i, carry):
            some = pl.ds(pl.multiple_of(i * GATED, GATED), GATED)
            gate, up = sums[some, :units], sums[some, units:]
            hidden[some] = (gate / (1.0 + jnp.exp(-gate)) * up).astype(jnp.bfloat16)
            return carry

        lax.fori_loop(0, hidden.shape[0] // GATED, gated, 0)
        load.wait()

        def lowered(i, carry):
            some = pl.ds(pl.multiple_of(i * COLUMNS, COLUMNS), COLUMNS)
            part = jnp.dot(
                hidden[...], down[:, some], preferred_element_type=jnp.float32
            ).astype(jnp.bfloat16)
            for j, target in enumerate(outs):
                target[:, some] = part[j * count : (j + 1) * count]
            return carry

        lax.fori_loop(0, down.shape[1] // COLUMNS, lowered, 0)


def expert(blocks, w_gate, w_up, w_down):
    count, model_width = blocks[0].shape
    units = w_gate.shape[1]
    total = len(blocks) * count
    whole = pl.BlockSpec((count, model_width), lambda i: (0, 0))
    deep = pl.BlockSpec((DEPTH, units), lambda i: (i, 0))
    out = jax.ShapeDtypeStruct((count, model_width), jnp.bfloat16)
    return pl.pallas_call(
        expert_kernel,
        grid=(model_width // DEPTH,),
        in_specs=[whole] * 4 + [deep, deep, pl.BlockSpec(memory_space=pl.ANY)],
        out_specs=[whole] * 4,
        out_shape=[out] * 4,
        scratch_shapes=[
            pltpu.VMEM((total, model_width), jnp.bfloat16),
            pltpu.VMEM((total, 2 * units), jnp.float32),
            pltpu.VMEM((total, units), jnp.bfloat16),
            pltpu.VMEM((units, model_width), jnp.bfloat16),
            pltpu.SemaphoreType.DMA,
        ],
        compiler_params=pltpu.CompilerParams(vmem_limit_bytes=FFN_LIMIT * 2**20),
        cost_estimate=pl.CostEstimate(
            flops=6 * total * model_width * units,
            bytes_accessed=6 * model_width * units + 4 * total * model_width,
            transcendentals=total * units,
        ),
    )(*blocks, w_gate, w_up, w_down)


def merge_kernel(*refs):
    parts, order, out = refs[:-2], refs[-2], refs[-1]
    half = len(parts) // 2
    width = out.shape[1]
    own, theirs = (
        jnp.concatenate([part[...] for part in some], axis=0).astype(jnp.float32)
        for some in (parts[:half], parts[half:])
    )
    total = (own + theirs).astype(jnp.bfloat16)
    stacked = jnp.concatenate(
        [total[:, first : first + width] for first in range(0, total.shape[1], width)], axis=0
    )
    out[...] = jnp.dot(order[...], stacked, preferred_element_type=jnp.float32).astype(jnp.bfloat16)


def merge(own, theirs, order, nz):
    count = sum(part.shape[0] for part in own)
    model_width = own[0].shape[1]
    width = model_width // SPLIT
    vmem = pl.BlockSpec(memory_space=pltpu.VMEM)
    packed = pl.pallas_call(
        merge_kernel,
        out_shape=jax.ShapeDtypeStruct((count * SPLIT, width), jnp.bfloat16),
        in_specs=[vmem] * (2 * len(own) + 1),
        out_specs=vmem,
        compiler_params=pltpu.CompilerParams(vmem_limit_bytes=12 * 2**20),
        cost_estimate=pl.CostEstimate(
            flops=2 * (count * SPLIT) ** 2 * width, bytes_accessed=8 * count * model_width, transcendentals=0
        ),
    )(*own, *theirs, order)
    return packed.reshape(nz, -1, width)


def through_row(packed, weights, capacity, pieces):
    rows = unpack(packed, capacity)
    size = rows.shape[0] // pieces
    cut = [rows[i * size : (i + 1) * size] for i in range(pieces)]
    own, theirs = [], []
    for mine in cut:
        partner = swap(mine, "x", 1)
        mine_other = swap(mine, "tp", 1)
        partner_other = swap(partner, "tp", 1)
        sums = expert((mine, partner, mine_other, partner_other), *weights)
        partner_half = add(sums[1], swap(sums[3], "tp", 1))
        own.append(add(sums[0], swap(sums[2], "tp", 1)))
        theirs.append(swap(partner_half, "x", 1))
    return own, theirs


def local(tokens, norm_gain, expert_ids, route_weights, w_gate, w_up, w_down):
    nz = lax.axis_size("z")
    expert_count = nz * ROW // 2
    tok_count, model_width = tokens.shape
    top_count = expert_ids.shape[1]
    capacity = 2 * max(1, 5 * tok_count * top_count // (8 * expert_count))
    width = model_width // SPLIT
    weights = (w_gate, w_up, w_down)
    pair = lax.axis_index("x") // 2

    values = tokens.astype(jnp.float32)
    scale_rows = lax.rsqrt(jnp.mean(values * values, axis=1, keepdims=True) + 1e-06)
    normed = (values * scale_rows * norm_gain).astype(jnp.bfloat16)
    stacked = jnp.concatenate(
        [normed[:, q * width : (q + 1) * width] for q in range(SPLIT)], axis=0
    )

    before = jnp.arange(tok_count)[:, None] > jnp.arange(tok_count)[None, :]
    places, parts = [], []
    for k in range(top_count):
        mine = expert_ids[:, k]
        same = sum((mine[:, None] == expert_ids[:, j][None, :]).astype(jnp.int32) for j in range(top_count))
        rank = jnp.sum(jnp.where(before, same, 0), axis=1)
        places.append((mine // 2) * capacity + rank)
        parts.append((mine % 2) ^ pair)

    line = jnp.arange(nz * SPLIT * capacity, dtype=jnp.int32)
    line_piece = (line // capacity) % SPLIT
    line_place = (line // (SPLIT * capacity)) * capacity + line % capacity
    piece = jnp.repeat(jnp.arange(SPLIT, dtype=jnp.int32), tok_count)

    def chosen(part, k):
        place = jnp.tile(jnp.where(parts[k] == part, places[k], -1), SPLIT)
        return (line_piece[:, None] == piece[None, :]) & (line_place[:, None] == place[None, :])

    def outgoing(part):
        select = chosen(part, 0)
        for k in range(1, top_count):
            select = select | chosen(part, k)
        message = jnp.dot(select.astype(jnp.bfloat16), stacked, preferred_element_type=jnp.float32)
        return message.astype(jnp.bfloat16).reshape(nz, SPLIT * capacity, width)

    stacked_piece = jnp.repeat(jnp.arange(SPLIT, dtype=jnp.int32), nz * capacity)
    stacked_place = jnp.tile(jnp.arange(nz * capacity, dtype=jnp.int32), SPLIT)
    order = (
        (line_piece[:, None] == stacked_piece[None, :]) & (line_place[:, None] == stacked_place[None, :])
    ).astype(jnp.bfloat16)

    near = along_z(outgoing(0))
    crossed = swap(outgoing(1), "x", 3)
    near, crossed, order = lax.optimization_barrier((near, crossed, order))
    far = along_z(crossed)

    own, theirs = through_row(near, weights, capacity, 2)
    near_out = merge(own, theirs, order, nz)
    far, near_out = lax.optimization_barrier((far, near_out))
    near_back = along_z(near_out)
    own, theirs = through_row(far, weights, capacity, 2)
    far_out = merge(own, theirs, order, nz)
    near_back, far_out = lax.optimization_barrier((near_back, far_out))
    far_back = along_z(far_out)
    far_back = swap(far_back, "x", 3)

    mixed = jnp.zeros((SPLIT * tok_count, width), jnp.float32)
    for k in range(top_count):
        picked = jnp.zeros((SPLIT * tok_count, width), jnp.float32)
        for part, back in ((0, near_back), (1, far_back)):
            select = chosen(part, k).T.astype(jnp.bfloat16)
            picked = picked + jnp.dot(
                select, back.reshape(-1, width), preferred_element_type=jnp.float32
            )
        mixed = mixed + picked * jnp.tile(route_weights[:, k], SPLIT)[:, None]
    mixed = mixed.astype(jnp.bfloat16)
    return jnp.concatenate(
        [mixed[q * tok_count : (q + 1) * tok_count] for q in range(SPLIT)], axis=1
    )


def solution(mesh):
    groups, ep, cores = (mesh.shape[name] for name in ("grp", "ep", "tp"))
    grid = Mesh(mesh.devices.reshape(groups, ep // ROW, ROW, cores), ("grp", "z", "x", "tp"))
    tok = P(("grp", "z", "x", "tp"), None)
    placed = (
        tok,
        P(),
        tok,
        tok,
        P(None, ("z", "x", "tp")),
        P(None, ("z", "x", "tp")),
        P(("z", "x", "tp"), None),
    )

    return jax.shard_map(local, mesh=grid, in_specs=placed, out_specs=tok, check_vma=False)
```

```python
import jax
import jax.numpy as jnp
from jax import lax
from jax.experimental import pallas as pl
from jax.experimental.pallas import tpu as pltpu
from jax.sharding import Mesh
from jax.sharding import PartitionSpec as P


ROW = 4
DEPTH = 512
GATED = 32
FFN_LIMIT = 50
COLUMNS = 1024
SPLIT = 4


def swap(block, axis, mask):
    count = lax.axis_size(axis)
    return lax.ppermute(block, axis, [(i, i ^ mask) for i in range(count)])


def unpack(packed, capacity):
    rows, _, width = packed.shape
    pieces = packed.reshape(rows, SPLIT, capacity, width)
    return pieces.transpose(0, 2, 1, 3).reshape(rows * capacity, SPLIT * width)


def along_z(packed):
    return lax.all_to_all(packed, "z", split_axis=0, concat_axis=0, tiled=True)


def add(a, b):
    return (a.astype(jnp.float32) + b.astype(jnp.float32)).astype(jnp.bfloat16)


def expert_kernel(*refs):
    ins, (w_gate, w_up, w_down), outs = refs[:4], refs[4:7], refs[7:11]
    rows, sums, hidden, down, sem = refs[11:]
    step, steps = pl.program_id(0), pl.num_programs(0)
    count, (depth, units) = ins[0].shape[0], w_gate.shape
    load = pltpu.make_async_copy(w_down, down, sem)

    @pl.when(step == 0)
    def _():
        load.start()
        for i, source in enumerate(ins):
            rows[i * count : (i + 1) * count] = source[...]
        sums[...] = jnp.zeros_like(sums)

    sums[...] += jnp.dot(
        rows[:, pl.ds(pl.multiple_of(step * depth, depth), depth)],
        jnp.concatenate([w_gate[...], w_up[...]], axis=1),
        preferred_element_type=jnp.float32,
    )

    @pl.when(step == steps - 1)
    def _():
        def gated(i, carry):
            some = pl.ds(pl.multiple_of(i * GATED, GATED), GATED)
            gate, up = sums[some, :units], sums[some, units:]
            hidden[some] = (gate / (1.0 + jnp.exp(-gate)) * up).astype(jnp.bfloat16)
            return carry

        lax.fori_loop(0, hidden.shape[0] // GATED, gated, 0)
        load.wait()

        def lowered(i, carry):
            some = pl.ds(pl.multiple_of(i * COLUMNS, COLUMNS), COLUMNS)
            part = jnp.dot(
                hidden[...], down[:, some], preferred_element_type=jnp.float32
            ).astype(jnp.bfloat16)
            for j, target in enumerate(outs):
                target[:, some] = part[j * count : (j + 1) * count]
            return carry

        lax.fori_loop(0, down.shape[1] // COLUMNS, lowered, 0)


def expert(blocks, w_gate, w_up, w_down):
    count, model_width = blocks[0].shape
    units = w_gate.shape[1]
    total = len(blocks) * count
    whole = pl.BlockSpec((count, model_width), lambda i: (0, 0))
    deep = pl.BlockSpec((DEPTH, units), lambda i: (i, 0))
    out = jax.ShapeDtypeStruct((count, model_width), jnp.bfloat16)
    return pl.pallas_call(
        expert_kernel,
        grid=(model_width // DEPTH,),
        in_specs=[whole] * 4 + [deep, deep, pl.BlockSpec(memory_space=pl.ANY)],
        out_specs=[whole] * 4,
        out_shape=[out] * 4,
        scratch_shapes=[
            pltpu.VMEM((total, model_width), jnp.bfloat16),
            pltpu.VMEM((total, 2 * units), jnp.float32),
            pltpu.VMEM((total, units), jnp.bfloat16),
            pltpu.VMEM((units, model_width), jnp.bfloat16),
            pltpu.SemaphoreType.DMA,
        ],
        compiler_params=pltpu.CompilerParams(vmem_limit_bytes=FFN_LIMIT * 2**20),
        cost_estimate=pl.CostEstimate(
            flops=6 * total * model_width * units,
            bytes_accessed=6 * model_width * units + 4 * total * model_width,
            transcendentals=total * units,
        ),
    )(*blocks, w_gate, w_up, w_down)


def merge_kernel(*refs):
    parts, order, out = refs[:-2], refs[-2], refs[-1]
    half = len(parts) // 2
    width = out.shape[1]
    own, theirs = (
        jnp.concatenate([part[...] for part in some], axis=0).astype(jnp.float32)
        for some in (parts[:half], parts[half:])
    )
    total = (own + theirs).astype(jnp.bfloat16)
    stacked = jnp.concatenate(
        [total[:, first : first + width] for first in range(0, total.shape[1], width)], axis=0
    )
    out[...] = jnp.dot(order[...], stacked, preferred_element_type=jnp.float32).astype(jnp.bfloat16)


def merge(own, theirs, order, nz):
    count = sum(part.shape[0] for part in own)
    model_width = own[0].shape[1]
    width = model_width // SPLIT
    vmem = pl.BlockSpec(memory_space=pltpu.VMEM)
    packed = pl.pallas_call(
        merge_kernel,
        out_shape=jax.ShapeDtypeStruct((count * SPLIT, width), jnp.bfloat16),
        in_specs=[vmem] * (2 * len(own) + 1),
        out_specs=vmem,
        compiler_params=pltpu.CompilerParams(vmem_limit_bytes=12 * 2**20),
        cost_estimate=pl.CostEstimate(
            flops=2 * (count * SPLIT) ** 2 * width, bytes_accessed=8 * count * model_width, transcendentals=0
        ),
    )(*own, *theirs, order)
    return packed.reshape(nz, -1, width)


def finish_kernel(mixed, back, *refs):
    selects, scales, out = refs[: len(refs) // 2], refs[len(refs) // 2 : -1], refs[-1]
    total = mixed[...]
    for select, scale in zip(selects, scales):
        picked = jnp.dot(select[...], back[...], preferred_element_type=jnp.float32)
        total = total + picked * scale[...]
    count, width = out.shape[0], total.shape[1]
    for q in range(SPLIT):
        out[:, q * width : (q + 1) * width] = total[q * count : (q + 1) * count].astype(out.dtype)


def finish(mixed, back, selects, scales):
    stacked, width = mixed.shape
    vmem = pl.BlockSpec(memory_space=pltpu.VMEM)
    return pl.pallas_call(
        finish_kernel,
        out_shape=jax.ShapeDtypeStruct((stacked // SPLIT, width * SPLIT), jnp.bfloat16),
        in_specs=[vmem] * (2 + 2 * len(selects)),
        out_specs=vmem,
        compiler_params=pltpu.CompilerParams(vmem_limit_bytes=16 * 2**20),
        cost_estimate=pl.CostEstimate(
            flops=2 * len(selects) * stacked * back.shape[0] * width,
            bytes_accessed=8 * stacked * width,
            transcendentals=0,
        ),
    )(mixed, back, *selects, *scales)


def through_row(packed, weights, capacity, pieces):
    rows = unpack(packed, capacity)
    size = rows.shape[0] // pieces
    cut = [rows[i * size : (i + 1) * size] for i in range(pieces)]
    own, theirs = [], []
    for mine in cut:
        partner = swap(mine, "x", 1)
        mine_other = swap(mine, "tp", 1)
        partner_other = swap(partner, "tp", 1)
        sums = expert((mine, partner, mine_other, partner_other), *weights)
        partner_half = add(sums[1], swap(sums[3], "tp", 1))
        own.append(add(sums[0], swap(sums[2], "tp", 1)))
        theirs.append(swap(partner_half, "x", 1))
    return own, theirs


def local(tokens, norm_gain, expert_ids, route_weights, w_gate, w_up, w_down):
    nz = lax.axis_size("z")
    expert_count = nz * ROW // 2
    tok_count, model_width = tokens.shape
    top_count = expert_ids.shape[1]
    capacity = 2 * max(1, 5 * tok_count * top_count // (8 * expert_count))
    width = model_width // SPLIT
    weights = (w_gate, w_up, w_down)
    pair = lax.axis_index("x") // 2

    values = tokens.astype(jnp.float32)
    scale_rows = lax.rsqrt(jnp.mean(values * values, axis=1, keepdims=True) + 1e-06)
    normed = (values * scale_rows * norm_gain).astype(jnp.bfloat16)
    stacked = jnp.concatenate(
        [normed[:, q * width : (q + 1) * width] for q in range(SPLIT)], axis=0
    )

    before = jnp.arange(tok_count)[:, None] > jnp.arange(tok_count)[None, :]
    places, parts = [], []
    for k in range(top_count):
        mine = expert_ids[:, k]
        same = sum((mine[:, None] == expert_ids[:, j][None, :]).astype(jnp.int32) for j in range(top_count))
        rank = jnp.sum(jnp.where(before, same, 0), axis=1)
        places.append((mine // 2) * capacity + rank)
        parts.append((mine % 2) ^ pair)

    line = jnp.arange(nz * SPLIT * capacity, dtype=jnp.int32)
    line_piece = (line // capacity) % SPLIT
    line_place = (line // (SPLIT * capacity)) * capacity + line % capacity
    piece = jnp.repeat(jnp.arange(SPLIT, dtype=jnp.int32), tok_count)

    def chosen(part, k):
        place = jnp.tile(jnp.where(parts[k] == part, places[k], -1), SPLIT)
        return (line_piece[:, None] == piece[None, :]) & (line_place[:, None] == place[None, :])

    def outgoing(part):
        select = chosen(part, 0)
        for k in range(1, top_count):
            select = select | chosen(part, k)
        message = jnp.dot(select.astype(jnp.bfloat16), stacked, preferred_element_type=jnp.float32)
        return message.astype(jnp.bfloat16).reshape(nz, SPLIT * capacity, width)

    stacked_piece = jnp.repeat(jnp.arange(SPLIT, dtype=jnp.int32), nz * capacity)
    stacked_place = jnp.tile(jnp.arange(nz * capacity, dtype=jnp.int32), SPLIT)
    order = (
        (line_piece[:, None] == stacked_piece[None, :]) & (line_place[:, None] == stacked_place[None, :])
    ).astype(jnp.bfloat16)

    near = along_z(outgoing(0))
    crossed = swap(outgoing(1), "x", 3)
    near, crossed, order = lax.optimization_barrier((near, crossed, order))
    far = along_z(crossed)

    own, theirs = through_row(near, weights, capacity, 2)
    near_out = merge(own, theirs, order, nz)
    far, near_out = lax.optimization_barrier((far, near_out))
    near_back = along_z(near_out)
    own, theirs = through_row(far, weights, capacity, 2)
    far_out = merge(own, theirs, order, nz)
    near_back, far_out = lax.optimization_barrier((near_back, far_out))
    far_back = along_z(far_out)
    far_back = swap(far_back, "x", 3)

    mixed = jnp.zeros((SPLIT * tok_count, width), jnp.float32)
    selects, scales = [], []
    for k in range(top_count):
        scale = jnp.tile(route_weights[:, k], SPLIT)[:, None]
        picked = jnp.dot(
            chosen(0, k).T.astype(jnp.bfloat16),
            near_back.reshape(-1, width),
            preferred_element_type=jnp.float32,
        )
        mixed = mixed + picked * scale
        place = jnp.tile(jnp.where(parts[k] == 1, places[k], -1), SPLIT)
        select = (line_piece[None, :] == piece[:, None]) & (line_place[None, :] == place[:, None])
        selects.append(select.astype(jnp.bfloat16))
        scales.append(scale)
    return finish(mixed, far_back.reshape(-1, width), selects, scales)


def solution(mesh):
    groups, ep, cores = (mesh.shape[name] for name in ("grp", "ep", "tp"))
    grid = Mesh(mesh.devices.reshape(groups, ep // ROW, ROW, cores), ("grp", "z", "x", "tp"))
    tok = P(("grp", "z", "x", "tp"), None)
    placed = (
        tok,
        P(),
        tok,
        tok,
        P(None, ("z", "x", "tp")),
        P(None, ("z", "x", "tp")),
        P(("z", "x", "tp"), None),
    )

    return jax.shard_map(local, mesh=grid, in_specs=placed, out_specs=tok, check_vma=False)
```
